128 devices in a mesh: rep: 2 (over z_hi), fs: 32 (over z_lo, y, x), tp: 2 (over core).
Axes of the slice: x: 4, y: 4, z: 4 (z_hi: 2, z_lo: 2; z = z_hi * 2 + z_lo), core: 2. Of those that a mesh axis runs over, the one named last changes fastest.
Arguments:
- tokens: bfloat16 [65536, 2048], P(('rep', 'fs', 'tp')), may hold values from -6 to 6
- pre_gain: bfloat16 [2048], replicated, may hold values from 0.099609375 to 1.8984375
- gate_weight: bfloat16 [2048, 2816], P('fs', 'tp'), may hold values from -0.125 to 0.125
- value_weight: bfloat16 [2048, 2816], P('fs', 'tp'), may hold values from -0.125 to 0.125
- down_weight: bfloat16 [2816, 2048], P('tp', 'fs'), may hold values from -0.109375 to 0.109375
- post_gain: bfloat16 [2048], replicated, may hold values from 0.099609375 to 1.8984375
Outputs:
- updated: bfloat16 [65536, 2048], P(('rep', 'fs', 'tp'))
The draws below stay inside these ranges and needn't reach their ends.
All inputs are finite; a program needn't handle non-finite values.
Results may differ from the reference program's by a relative error of at most 0.0055.
Values may be sent and summed in bfloat16 or wider, within the bound.
No kernel may reach another device: no remote copies, remote signals or barrier semaphores. Data moves between devices by JAX's collectives and lax.ppermute only.
A program may use at most 128 MiB of HBM per device.

```python
import jax
import jax.numpy as jnp
from jax import lax

D = 2048
FF = 2816
TOK_DEV = 512
TOKENS = 65536
N_REP = 2
N_FS = 32
N_TP = 2


def block_levels(own_key, dims, cuts, low, largest):
    def one(axis_at, shards_of):
        draws = jax.random.uniform(jax.random.fold_in(jax.random.fold_in(own_key, 6), axis_at), (shards_of,), jnp.float32, low / len(cuts), largest / len(cuts))
        return jnp.repeat(jnp.exp(draws), dims[axis_at] // shards_of).reshape((-1,) + (1,) * (len(dims) - axis_at - 1))

    level = one(*cuts[0])
    for cut in cuts[1:]:
        level = level * one(*cut)
    return level


def centred(own_key, extent, scale, limit, shards=(), held_as=jnp.bfloat16):
    entries = jax.random.normal(own_key, extent, jnp.float32) * scale
    if len(shards) > 0:
        entries = block_levels(own_key, extent, shards, -0.22, 0.18) * entries
    return jnp.clip(entries, min=-limit, max=limit).astype(held_as)


def setup_inputs(seed: int = 0) -> dict:
    key_list = jax.random.split(jax.random.key(seed), 7)
    return {
        "tokens": centred(key_list[0], (TOKENS, D), 1.0, 6.0, ((0, 128),)),
        "pre_gain": jnp.clip(1.0 + 0.18 * jax.random.normal(key_list[1], (D,), jnp.float32), 0.099609375, 1.8984375).astype(jnp.bfloat16),
        "gate_weight": centred(key_list[2], (D, FF), D ** -0.5, 0.125, ((0, 32), (1, 2))),
        "value_weight": centred(key_list[3], (D, FF), D ** -0.5, 0.125, ((0, 32), (1, 2))),
        "down_weight": centred(key_list[4], (FF, D), FF ** -0.5, 0.109375, ((0, 2), (1, 32))),
        "post_gain": jnp.clip(1.0 + 0.18 * jax.random.normal(key_list[5], (D,), jnp.float32), 0.099609375, 1.8984375).astype(jnp.bfloat16),
    }


eps_norm = 1e-06

def rms_rows(values_in, gain):
    floats = values_in.astype(jnp.float32)
    scaled = floats * lax.rsqrt(lax.optimization_barrier(jnp.mean(floats * floats, -1, keepdims=True)) + eps_norm)
    return scaled * gain.astype(jnp.float32)

def reference(tokens, pre_gain, gate_weight, value_weight, down_weight, post_gain):
    group_size = TOK_DEV * N_TP
    block_width = FF // N_TP
    grouped = tokens.reshape(N_REP * N_FS, group_size, D)

    def one_group(block_rows):
        normed = rms_rows(block_rows, pre_gain).astype(jnp.bfloat16)
        gate_proj = jnp.dot(normed, gate_weight, preferred_element_type=jnp.float32)
        value_proj = jnp.dot(normed, value_weight, preferred_element_type=jnp.float32)
        hidden = (jax.nn.silu(gate_proj) * value_proj).astype(jnp.bfloat16)
        total = jnp.zeros((group_size, D), jnp.float32)
        for block_index in range(N_TP):
            lower = block_index * block_width
            partial_term = jnp.dot(hidden[:, lower:lower + block_width], down_weight[lower:lower + block_width], preferred_element_type=jnp.float32).astype(jnp.bfloat16)
            total = total + lax.optimization_barrier(partial_term).astype(jnp.float32)
        branch = total.astype(jnp.bfloat16)
        return (block_rows.astype(jnp.float32) + 0.5 * rms_rows(branch, post_gain)).astype(jnp.bfloat16)
    return lax.map(one_group, grouped).reshape(TOKENS, D)
```

```python
import jax
import jax.numpy as jnp
from jax import lax
from jax.sharding import Mesh
from jax.sharding import PartitionSpec as P

FS = ("fs_0", "fs_1", "fs_2")
REP_FS = ("rep", "fs_0", "fs_1", "fs_2")
REP_FS_TP = ("rep", "fs_0", "fs_1", "fs_2", "tp")

eps_norm = 1e-06
SWAP = [(0, 1), (1, 0)]


def rms_rows(values_in, gain):
    floats = values_in.astype(jnp.float32)
    scaled = floats * lax.rsqrt(jnp.mean(floats * floats, -1, keepdims=True) + eps_norm)
    return scaled * gain.astype(jnp.float32)


def shards(tokens, pre_gain, gate_weight, value_weight, down_weight, post_gain):
    rep = lax.axis_index("rep")
    down_rows = down_weight.T
    half = down_rows.shape[0] // 2
    own = jnp.where(rep == 0, gate_weight, value_weight)
    own_down = lax.dynamic_slice_in_dim(down_rows, rep * half, half, 0)
    sent = jnp.concatenate([own, own_down], 0)
    rows = own.shape[0]
    whole = lax.all_gather(sent, REP_FS, axis=0)
    whole = whole.reshape(2, -1, *sent.shape)
    gate = whole[0, :, :rows].reshape(-1, sent.shape[1])
    value = whole[1, :, :rows].reshape(-1, sent.shape[1])
    down = whole[:, :, rows:].swapaxes(0, 1).reshape(-1, sent.shape[1])

    normed = rms_rows(tokens, pre_gain).astype(jnp.bfloat16)
    other = lax.ppermute(normed, "tp", SWAP)

    def partial(rows_in):
        gate_add = jnp.dot(rows_in, gate, preferred_element_type=jnp.float32)
        value_add = jnp.dot(rows_in, value, preferred_element_type=jnp.float32)
        hidden = (jax.nn.silu(gate_add) * value_add).astype(jnp.bfloat16)
        return lax.dot_general(
            hidden, down, (((1,), (1,)), ((), ())), preferred_element_type=jnp.float32
        ).astype(jnp.bfloat16)

    theirs = lax.ppermute(partial(other), "tp", SWAP)
    mine = partial(normed)
    branch = (mine.astype(jnp.float32) + theirs.astype(jnp.float32)).astype(jnp.bfloat16)
    updated = tokens.astype(jnp.float32) + 0.5 * rms_rows(branch, post_gain)
    return updated.astype(jnp.bfloat16)


def solution(mesh):
    torus = Mesh(
        mesh.devices.reshape(mesh.shape["rep"], 2, 4, 4, mesh.shape["tp"]),
        ("rep", "fs_0", "fs_1", "fs_2", "tp"),
    )
    in_specs = (P(REP_FS_TP, None), P(), P(FS, "tp"), P(FS, "tp"), P("tp", FS), P())
    out_specs = P(REP_FS_TP, None)
    return jax.shard_map(
        shards, mesh=torus, in_specs=in_specs, out_specs=out_specs, check_vma=False
    )
```
